32 devices in a mesh: fs: 8 (over z, y), tp: 4 (over x, core).
Axes of the slice: x: 2, y: 2, z: 4, core: 2. Of those that a mesh axis runs over, the one named last changes fastest.
Arguments:
- tokens: bfloat16 [8192, 2048], P('fs'), may hold values from -6 to 6
- norm_gain: float32 [2048], P('fs'), may hold values from 0.1 to 1.9
- gate_train: float32 [8, 2048, 768], P(None, 'fs', 'tp'), may hold values from -0.125 to 0.125
- up_train: float32 [8, 2048, 768], P(None, 'fs', 'tp'), may hold values from -0.125 to 0.125
- down_train: float32 [8, 768, 2048], P(None, 'fs', 'tp'), may hold values from -0.21875 to 0.21875
- expert_ids: int32 [8192, 2], P('fs'), may hold values from 0 to 7, all different within a row; in each aligned block of 1024 rows (0 to 1023, 1024 to 2047, ...) at most 512 rows name the same one
- route_weights: float32 [8192, 2], P('fs'), may hold values from 0.1 to 1
Outputs:
- gate_serve: bfloat16 [8, 2048, 768], P('fs', None, 'tp')
- up_serve: bfloat16 [8, 2048, 768], P('fs', None, 'tp')
- down_serve: bfloat16 [8, 768, 2048], P('fs', 'tp')
- mixed: bfloat16 [8192, 2048], P('fs', 'tp')
The draws below stay inside these ranges and needn't reach their ends.
Inputs may be any that keep to these rules, and one draw needn't show every extreme that they name: `expert_ids`: each row names 2 different experts. Within each aligned block of 1024 rows no expert is named more than 512 times, and in every block some expert is named exactly 512 times; every expert is named somewhere.
All inputs are finite; a program needn't handle non-finite values.
Results may differ from the reference program's by a relative error of at most 0.011.
Values may be sent and summed in bfloat16 or wider, within the bound.
No kernel may reach another device: no remote copies, remote signals or barrier semaphores. Data moves between devices by JAX's collectives and lax.ppermute only.
A program may use at most 128 MiB of HBM per device.

```python
import math
import jax
import jax.numpy as jnp
import numpy as np
from jax import lax

D = 2048
FF = 768
TOP = 2
TOK_DEV = 1024
EXPERTS = 8
CAP = 512
TOKENS = 8192
N_FS = 8
N_TP = 4


def shard_levels(key, shape, shards, least, top_value):
    loudness = 1.0
    for axis_at, parts in shards:
        draws = jax.random.uniform(jax.random.fold_in(jax.random.fold_in(key, 6), axis_at), (parts,), jnp.float32, least / len(shards), top_value / len(shards))
        loudness = loudness * jnp.repeat(jnp.exp(draws), shape[axis_at] // parts).reshape((-1,) + (1,) * (len(shape) - 1 - axis_at))
    return loudness


def shared_out(own_key, own, number, rows, number_of, top, limit, lean):
    ranking = jax.random.permutation(own_key, number_of)
    heavy_load, ordinary = portions_of(number_of, rows * top, limit, lean, True), portions_of(number_of, rows * top, limit, lean, False)
    places = jnp.arange(number_of)

    def named(sizes, offset_by):
        used = int((sizes > 0).sum())
        fixed = max(1, used // 4)
        moved = fixed + (places - fixed + offset_by * (used - fixed)) % max(1, number_of - fixed)
        return jnp.zeros((number_of,), jnp.int32).at[ranking[jnp.where(places < fixed, places, moved)]].set(jnp.asarray(sizes, jnp.int32))

    sizes = jnp.where(number % 4 == 0, named(heavy_load, number // 4), named(ordinary, number - number // 4 - 1))
    mixed = jax.random.permutation(jax.random.fold_in(own, 3), number_of)
    source_of, sink = mixed[0:number_of // 2 * 2:2], mixed[1:number_of // 2 * 2:2]
    slack = jnp.minimum(sizes[source_of] - 1, limit - sizes[sink]) // 2
    slack = jnp.where((source_of == ranking[0]) | (sink == ranking[0]) | (sizes[sink] == 0), 0, jnp.maximum(slack, 0))
    moved = jax.random.randint(jax.random.fold_in(own, 4), (number_of // 2,), 0, 1 << 20) % (slack + 1)
    sizes = sizes.at[source_of].add(-moved).at[sink].add(moved)
    items = jnp.searchsorted(jnp.cumsum(sizes), jnp.arange(rows * top), side="right").astype(jnp.int32)
    table = items.reshape(top, rows).T
    table = table[jax.random.permutation(jax.random.fold_in(own, 1), rows)]
    offset_by = jax.random.randint(jax.random.fold_in(own, 2), (rows, 1), 0, top)
    return jnp.take_along_axis(table, (jnp.arange(top)[None, :] + offset_by) % top, axis=1)


def portions_of(number_of, total, limit, slope, full):
    portions = [(1 << 20) // math.isqrt(standing ** slope) + 1 for standing in range(1, number_of + 1)]
    largest = limit if full else min(limit, max(-(-total // number_of), total * portions[0] // sum(portions)))
    least = 1 if total - largest >= number_of - 1 else 0
    counts, rest = [largest] + [least] * (number_of - 1), total - largest - least * (number_of - 1)
    while rest > 0:
        movable = [i for i in range(1, number_of) if counts[i] < largest] or [i for i in range(1, number_of) if counts[i] < limit]
        mass, budget = sum([portions[i] for i in movable]), rest
        for i in movable:
            addition = min(limit - counts[i], max(1, budget * portions[i] // mass), rest)
            counts[i] = counts[i] + addition
            rest = rest - addition
    return np.array(counts)


def bell_draw(rng, dims, spread, reach, pieces=(), held_as=jnp.bfloat16):
    entries = jax.random.normal(rng, dims, jnp.float32) * spread
    if len(pieces) > 0:
        entries = shard_levels(rng, dims, pieces, -0.22, 0.18) * entries
    return jnp.clip(entries, min=-reach, max=reach).astype(held_as)


def setup_inputs(seed: int = 0) -> dict:
    keys = jax.random.split(jax.random.key(seed), 8)
    tokens = bell_draw(keys[0], (TOKENS, D), 1.0, 6.0, ((0, 8),))
    norm_gain = jnp.clip(1.0 + 0.18 * jax.random.normal(keys[1], (D,), jnp.float32), 0.1, 1.9)
    gate_train = bell_draw(keys[2], (EXPERTS, D, FF), D ** -0.5, 0.125, ((1, 8), (2, 4)), jnp.float32)
    up_train = bell_draw(keys[3], (EXPERTS, D, FF), D ** -0.5, 0.125, ((1, 8), (2, 4)), jnp.float32)
    down_train = bell_draw(keys[4], (EXPERTS, FF, D), FF ** -0.5, 0.21875, ((1, 8), (2, 4)), jnp.float32)
    expert_ids_keys = jax.random.split(jax.random.fold_in(keys[5], 1), TOKENS // TOK_DEV)
    expert_ids_turns = jax.random.permutation(jax.random.fold_in(keys[5], 3), TOKENS // TOK_DEV)
    expert_ids = jax.vmap(lambda own, number: shared_out(jax.random.fold_in(keys[5], 2), own, number, TOK_DEV, EXPERTS, TOP, CAP, 2))(expert_ids_keys, expert_ids_turns).reshape((TOKENS, TOP))
    route_weights = jnp.clip(jnp.exp(math.log(1.0) - 2.3025851 * jax.random.uniform(keys[6], (TOKENS, TOP), jnp.float32) ** shard_levels(keys[6], (TOKENS, TOP), ((0, 8),), -0.2, 0.2)), 0.1, 1.0)
    return dict(tokens=tokens, norm_gain=norm_gain, gate_train=gate_train, up_train=up_train, down_train=down_train, expert_ids=expert_ids, route_weights=route_weights)


epsilon = 1e-06

def reference(tokens, norm_gain, gate_train, up_train, down_train, expert_ids, route_weights):
    gate_serve = (norm_gain[None, :, None] * gate_train).astype(jnp.bfloat16)
    up_serve = (norm_gain[None, :, None] * up_train).astype(jnp.bfloat16)
    down_serve = down_train.astype(jnp.bfloat16)
    tok_float = tokens.astype(jnp.float32)
    normed = (tok_float * lax.rsqrt(lax.optimization_barrier(jnp.mean(tok_float * tok_float, axis=-1, keepdims=True)) + epsilon)).astype(jnp.bfloat16)
    flat_ids = expert_ids.reshape(N_FS, TOK_DEV * TOP)
    onehot = (flat_ids[:, :, None] == jnp.arange(EXPERTS, dtype=jnp.int32)[None, None, :]).astype(jnp.int32)
    slot_rank = lax.optimization_barrier(jnp.sum((jnp.cumsum(onehot, axis=1) - onehot) * onehot, axis=-1))
    row_index = (jnp.arange(N_FS, dtype=jnp.int32)[:, None] * CAP + slot_rank).astype(jnp.int32)
    tok_index = (jnp.arange(N_FS, dtype=jnp.int32)[:, None] * TOK_DEV + jnp.arange(TOK_DEV * TOP, dtype=jnp.int32)[None, :] // TOP).astype(jnp.int32)
    buffer = jnp.zeros((EXPERTS, N_FS * CAP, D), jnp.bfloat16)
    buffer = buffer.at[flat_ids.reshape(-1), row_index.reshape(-1)].set(normed[tok_index.reshape(-1)])
    block_width = FF // N_TP

    def expert_apply(inputs):
        routed, weight_gate, weight_up, weight_down = inputs
        gate_act = jnp.dot(routed, weight_gate, preferred_element_type=jnp.float32)
        up_act = jnp.dot(routed, weight_up, preferred_element_type=jnp.float32)
        hidden = (jax.nn.silu(gate_act) * up_act).astype(jnp.bfloat16)
        running = jnp.zeros((routed.shape[0], D), jnp.float32)
        for index_tp in range(N_TP):
            partial_value = jnp.dot(hidden[:, index_tp * block_width:(index_tp + 1) * block_width], weight_down[index_tp * block_width:(index_tp + 1) * block_width], preferred_element_type=jnp.float32)
            running = running + partial_value.astype(jnp.bfloat16).astype(jnp.float32)
        return running.astype(jnp.bfloat16)
    outputs = lax.map(expert_apply, (buffer, gate_serve, up_serve, down_serve))
    picked = outputs[flat_ids.reshape(-1), row_index.reshape(-1)].reshape(TOKENS, TOP, D).astype(jnp.float32)
    shares = route_weights / lax.optimization_barrier(jnp.sum(route_weights, axis=-1, keepdims=True))
    mixed = lax.optimization_barrier(jnp.sum(shares[:, :, None] * picked, axis=1)).astype(jnp.bfloat16)
    return (gate_serve, up_serve, down_serve, mixed)
```

```python
import jax
import jax.numpy as jnp
from jax import lax
from jax.experimental import pallas as pl
from jax.experimental.pallas import tpu as pltpu
from jax.sharding import PartitionSpec as P

epsilon = 1e-06


def hidden_kernel(rows_ref, gate_ref, up_ref, hidden_ref):
    rows = rows_ref[...]
    across = (((1,), (1,)), ((), ()))
    gate_act = lax.dot_general(rows, gate_ref[...], across, preferred_element_type=jnp.float32)
    up_act = lax.dot_general(rows, up_ref[...], across, preferred_element_type=jnp.float32)
    hidden_ref[...] = (gate_act / (1.0 + jnp.exp(-gate_act)) * up_act).astype(jnp.bfloat16)


def down_kernel(hidden_ref, down_ref, out_ref):
    hidden = hidden_ref[...]
    sources, shares, rows, width = out_ref.shape
    for share in range(shares):
        value = jnp.dot(hidden, down_ref[share], preferred_element_type=jnp.float32)
        out_ref[:, share] = value.astype(jnp.bfloat16).reshape(sources, rows, width)


def expert_hidden(rows, gate_t, up_t, step):
    count, width = rows.shape
    units = gate_t.shape[0]
    return pl.pallas_call(
        hidden_kernel,
        grid=(count // step,),
        in_specs=[
            pl.BlockSpec((step, width), lambda i: (i, 0)),
            pl.BlockSpec((units, width), lambda i: (0, 0)),
            pl.BlockSpec((units, width), lambda i: (0, 0)),
        ],
        out_specs=pl.BlockSpec((step, units), lambda i: (i, 0)),
        out_shape=jax.ShapeDtypeStruct((count, units), jnp.bfloat16),
        cost_estimate=pl.CostEstimate(
            flops=4 * count * units * width,
            transcendentals=count * units,
            bytes_accessed=2 * (count * width + 2 * units * width + count * units),
        ),
        name="expert_hidden",
    )(rows, gate_t, up_t)


def expert_out(hidden, down, sources, step_sources):
    count, units = hidden.shape
    shares, _, width = down.shape
    rows = count // sources
    return pl.pallas_call(
        down_kernel,
        grid=(sources // step_sources,),
        in_specs=[
            pl.BlockSpec((step_sources * rows, units), lambda i: (i, 0)),
            pl.BlockSpec((shares, units, width), lambda i: (0, 0, 0)),
        ],
        out_specs=pl.BlockSpec((step_sources, shares, rows, width), lambda i: (i, 0, 0, 0)),
        out_shape=jax.ShapeDtypeStruct((sources, shares, rows, width), jnp.bfloat16),
        cost_estimate=pl.CostEstimate(
            flops=2 * count * units * width * shares,
            transcendentals=0,
            bytes_accessed=2 * (count * units + shares * units * width + count * width * shares),
        ),
        name="expert_out",
    )(hidden, down)


def on_device(tokens, norm_gain, gate_train, up_train, down_train, expert_ids, route_weights):
    fs_count = lax.axis_size("fs")
    tp_count = lax.axis_size("tp")
    tp_index = lax.axis_index("tp")
    experts, own_rows, own_units = gate_train.shape
    assert experts == fs_count
    down_rows, down_width = down_train.shape[1:]
    tok_rows, picks = expert_ids.shape
    width = tokens.shape[1]
    capacity = 2 * tok_rows * picks // experts
    quarter = capacity // tp_count

    gain = norm_gain[None, None, :]
    gate_cast = (gain * jnp.swapaxes(gate_train, 1, 2)).astype(jnp.bfloat16)
    up_cast = (gain * jnp.swapaxes(up_train, 1, 2)).astype(jnp.bfloat16)
    down_cast = down_train.astype(jnp.bfloat16)
    cuts = down_width // own_rows
    down_cut = jnp.concatenate(
        [down_cast[:, :, cut * own_rows : (cut + 1) * own_rows] for cut in range(cuts)], axis=1
    )
    packed = jnp.concatenate([gate_cast, up_cast, down_cut], axis=1)
    arrived = lax.all_to_all(packed, "fs", split_axis=0, concat_axis=0, tiled=True)

    tok_float = tokens.astype(jnp.float32)
    normed = (
        tok_float * lax.rsqrt(jnp.mean(tok_float * tok_float, axis=-1, keepdims=True) + epsilon)
    ).astype(jnp.bfloat16)
    flat_ids = expert_ids.reshape(-1)
    onehot = (flat_ids[:, None] == jnp.arange(experts, dtype=jnp.int32)[None, :]).astype(jnp.int32)
    slot_rank = jnp.sum((jnp.cumsum(onehot, axis=0) - onehot) * onehot, axis=1)
    target = (flat_ids * capacity + slot_rank).reshape(tok_rows, picks)
    own_slots = (
        jnp.arange(experts, dtype=jnp.int32)[:, None] * capacity
        + tp_index * quarter
        + jnp.arange(quarter, dtype=jnp.int32)[None, :]
    ).reshape(-1)
    named = own_slots[:, None] == target[None, :, 0]
    for pick in range(1, picks):
        named = named | (own_slots[:, None] == target[None, :, pick])
    outgoing = jnp.dot(
        named.astype(jnp.bfloat16), normed, preferred_element_type=jnp.float32
    ).astype(jnp.bfloat16)
    outgoing = outgoing.reshape(experts, quarter, width)
    outgoing, arrived = lax.optimization_barrier((outgoing, arrived))
    routed = lax.all_to_all(outgoing, "fs", split_axis=0, concat_axis=0, tiled=True)

    def joined(part):
        return jnp.swapaxes(part, 0, 1).reshape(part.shape[1], fs_count * own_rows)

    gate_t = joined(arrived[:, :own_units])
    up_t = joined(arrived[:, own_units : 2 * own_units])
    down_own = jnp.concatenate(
        [
            arrived[
                :, 2 * own_units + cut * down_rows : 2 * own_units + (cut + 1) * down_rows
            ].reshape(fs_count * down_rows, own_rows)
            for cut in range(cuts)
        ],
        axis=1,
    )
    gate_whole = lax.all_gather(gate_t, "tp", axis=0, tiled=True)
    up_whole = lax.all_gather(up_t, "tp", axis=0, tiled=True)
    down_whole = lax.all_gather(down_own, "tp", axis=0, tiled=False)
    gate_serve = jnp.swapaxes(gate_t, 0, 1)[None]
    up_serve = jnp.swapaxes(up_t, 0, 1)[None]
    units_share = down_own.shape[0] // tp_count
    down_serve = lax.dynamic_slice_in_dim(down_whole, tp_index * units_share, units_share, 1)
    down_serve = jnp.swapaxes(down_serve, 0, 1).reshape(1, units_share, width)

    step_sources = max(1, 256 // quarter)
    hidden = expert_hidden(
        routed.reshape(fs_count * quarter, width), gate_whole, up_whole, step_sources * quarter
    )
    results = expert_out(hidden, down_whole, fs_count, step_sources)
    returned = lax.all_to_all(
        results.reshape(fs_count * tp_count, quarter, down_width),
        ("fs", "tp"),
        split_axis=0,
        concat_axis=0,
        tiled=True,
    ).reshape(experts * capacity, down_width)

    shares = route_weights / jnp.sum(route_weights, axis=-1, keepdims=True)
    slot_ids = jnp.arange(experts * capacity, dtype=jnp.int32)
    mixing = jnp.zeros((tok_rows, experts * capacity), jnp.float32)
    for pick in range(picks):
        mixing = jnp.where(
            target[:, pick][:, None] == slot_ids[None, :], shares[:, pick][:, None], mixing
        )
    mixed = jnp.dot(
        mixing.astype(jnp.bfloat16), returned, preferred_element_type=jnp.float32
    )
    return (gate_serve, up_serve, down_serve, mixed.astype(jnp.bfloat16))


def solution(mesh):
    return jax.shard_map(
        on_device,
        mesh=mesh,
        in_specs=(
            P("fs", None),
            P("fs"),
            P(None, "fs", "tp"),
            P(None, "fs", "tp"),
            P(None, "fs", "tp"),
            P("fs", None),
            P("fs", None),
        ),
        out_specs=(P("fs", None, "tp"), P("fs", None, "tp"), P("fs", "tp", None), P("fs", "tp")),
        check_vma=False,
    )
```

```python
import jax
import jax.numpy as jnp
from jax import lax
from jax.experimental import pallas as pl
from jax.experimental.pallas import tpu as pltpu
from jax.sharding import PartitionSpec as P

epsilon = 1e-06


def hidden_kernel(first_ref, rows_ref, gate_ref, up_ref, hidden_ref):
    rows = rows_ref[...]
    across = (((1,), (1,)), ((), ()))
    gate_act = lax.dot_general(rows, gate_ref[...], across, preferred_element_type=jnp.float32)
    up_act = lax.dot_general(rows, up_ref[...], across, preferred_element_type=jnp.float32)
    hidden_ref[...] = (gate_act / (1.0 + jnp.exp(-gate_act)) * up_act).astype(jnp.bfloat16)


def down_kernel(hidden_ref, down_ref, out_ref):
    hidden = hidden_ref[...]
    sources, shares, rows, width = out_ref.shape
    for share in range(shares):
        value = jnp.dot(hidden, down_ref[share], preferred_element_type=jnp.float32)
        out_ref[:, share] = value.astype(jnp.bfloat16).reshape(sources, rows, width)


def expert_hidden(first, rows, gate_t, up_t, step):
    width = rows.shape[1]
    count = rows.shape[0] // 2
    units = gate_t.shape[0]
    return pl.pallas_call(
        hidden_kernel,
        grid_spec=pltpu.PrefetchScalarGridSpec(
            num_scalar_prefetch=1,
            grid=(count // step,),
            in_specs=[
                pl.BlockSpec((step, width), lambda i, first_ref: (first_ref[0] + i, 0)),
                pl.BlockSpec((units, width), lambda i, first_ref: (0, 0)),
                pl.BlockSpec((units, width), lambda i, first_ref: (0, 0)),
            ],
            out_specs=pl.BlockSpec((step, units), lambda i, first_ref: (i, 0)),
        ),
        out_shape=jax.ShapeDtypeStruct((count, units), jnp.bfloat16),
        cost_estimate=pl.CostEstimate(
            flops=4 * count * units * width,
            transcendentals=count * units,
            bytes_accessed=2 * (count * width + 2 * units * width + count * units),
        ),
        name="expert_hidden",
    )(first, rows, gate_t, up_t)


def expert_out(hidden, down, sources, step_sources):
    count, units = hidden.shape
    shares, _, width = down.shape
    rows = count // sources
    return pl.pallas_call(
        down_kernel,
        grid=(sources // step_sources,),
        in_specs=[
            pl.BlockSpec((step_sources * rows, units), lambda i: (i, 0)),
            pl.BlockSpec((shares, units, width), lambda i: (0, 0, 0)),
        ],
        out_specs=pl.BlockSpec((step_sources, shares, rows, width), lambda i: (i, 0, 0, 0)),
        out_shape=jax.ShapeDtypeStruct((sources, shares, rows, width), jnp.bfloat16),
        cost_estimate=pl.CostEstimate(
            flops=2 * count * units * width * shares,
            transcendentals=0,
            bytes_accessed=2 * (count * units + shares * units * width + count * width * shares),
        ),
        name="expert_out",
    )(hidden, down)


def on_device(tokens, norm_gain, gate_train, up_train, down_train, expert_ids, route_weights):
    fs_count = lax.axis_size("fs")
    tp_count = lax.axis_size("tp")
    tp_index = lax.axis_index("tp")
    experts, own_rows, own_units = gate_train.shape
    assert experts == fs_count
    down_rows, down_width = down_train.shape[1:]
    tok_rows, picks = expert_ids.shape
    width = tokens.shape[1]
    capacity = 2 * tok_rows * picks // experts
    quarter = capacity // tp_count

    gain = norm_gain[None, None, :]
    gate_cast = (gain * jnp.swapaxes(gate_train, 1, 2)).astype(jnp.bfloat16)
    up_cast = (gain * jnp.swapaxes(up_train, 1, 2)).astype(jnp.bfloat16)
    down_cast = down_train.astype(jnp.bfloat16)
    cuts = down_width // own_rows
    down_cut = jnp.concatenate(
        [down_cast[:, :, cut * own_rows : (cut + 1) * own_rows] for cut in range(cuts)], axis=1
    )
    packed = jnp.concatenate([gate_cast, up_cast, down_cut], axis=1)
    arrived = lax.all_to_all(packed, "fs", split_axis=0, concat_axis=0, tiled=True)

    tok_float = tokens.astype(jnp.float32)
    normed = (
        tok_float * lax.rsqrt(jnp.mean(tok_float * tok_float, axis=-1, keepdims=True) + epsilon)
    ).astype(jnp.bfloat16)
    flat_ids = expert_ids.reshape(-1)
    onehot = (flat_ids[:, None] == jnp.arange(experts, dtype=jnp.int32)[None, :]).astype(jnp.int32)
    slot_rank = jnp.sum((jnp.cumsum(onehot, axis=0) - onehot) * onehot, axis=1)
    target = (flat_ids * capacity + slot_rank).reshape(tok_rows, picks)
    own_slots = (
        jnp.arange(experts, dtype=jnp.int32)[:, None] * capacity
        + tp_index * quarter
        + jnp.arange(quarter, dtype=jnp.int32)[None, :]
    ).reshape(-1)
    named = own_slots[:, None] == target[None, :, 0]
    for pick in range(1, picks):
        named = named | (own_slots[:, None] == target[None, :, pick])
    outgoing = jnp.dot(
        named.astype(jnp.bfloat16), normed, preferred_element_type=jnp.float32
    ).astype(jnp.bfloat16)
    outgoing = outgoing.reshape(experts, quarter, width)
    outgoing, arrived = lax.optimization_barrier((outgoing, arrived))
    routed = lax.all_to_all(outgoing, "fs", split_axis=0, concat_axis=0, tiled=True)

    def joined(part):
        return jnp.swapaxes(part, 0, 1).reshape(part.shape[1], fs_count * own_rows)

    gate_t = joined(arrived[:, :own_units])
    up_t = joined(arrived[:, own_units : 2 * own_units])
    down_own = jnp.concatenate(
        [
            arrived[
                :, 2 * own_units + cut * down_rows : 2 * own_units + (cut + 1) * down_rows
            ].reshape(fs_count * down_rows, own_rows)
            for cut in range(cuts)
        ],
        axis=1,
    )
    gate_whole = lax.all_gather(gate_t, "tp", axis=0, tiled=True)
    up_whole = lax.all_gather(up_t, "tp", axis=0, tiled=True)
    down_whole = lax.all_gather(down_own, "tp", axis=0, tiled=False)
    gate_serve = jnp.swapaxes(gate_t, 0, 1)[None]
    up_serve = jnp.swapaxes(up_t, 0, 1)[None]
    units_share = down_own.shape[0] // tp_count
    down_serve = lax.dynamic_slice_in_dim(down_whole, tp_index * units_share, units_share, 1)
    down_serve = jnp.swapaxes(down_serve, 0, 1).reshape(1, units_share, width)

    half = fs_count // 2
    assert 2 * half == fs_count
    own_half = lax.axis_index("fs") // half
    mirror = [(source, (source + half) % fs_count) for source in range(fs_count)]
    members = half * tp_count
    halves = [list(range(members)), list(range(members, 2 * members))]
    half_slots = half * capacity
    step_sources = min(half, max(1, 256 // quarter))
    rows = routed.reshape(fs_count * quarter, width)
    blocks = half // step_sources

    def apply_half(which, rows):
        first = (which * blocks).astype(jnp.int32).reshape(1)
        hidden = expert_hidden(first, rows, gate_whole, up_whole, step_sources * quarter)
        return expert_out(hidden, down_whole, half, step_sources)

    def spread(results):
        return lax.all_to_all(
            results.reshape(members, quarter, down_width),
            ("fs", "tp"),
            split_axis=0,
            concat_axis=0,
            axis_index_groups=halves,
            tiled=True,
        ).reshape(half_slots, down_width)

    slot_ids = own_half * half_slots + jnp.arange(half_slots, dtype=jnp.int32)

    def mix(target, shares, values):
        mixing = jnp.zeros((tok_rows, half_slots), jnp.float32)
        for pick in range(picks):
            mixing = jnp.where(
                target[:, pick][:, None] == slot_ids[None, :], shares[:, pick][:, None], mixing
            )
        return jnp.dot(mixing.astype(jnp.bfloat16), values, preferred_element_type=jnp.float32)

    shares = route_weights / jnp.sum(route_weights, axis=-1, keepdims=True)
    mirror_target = lax.ppermute(target, "fs", mirror)
    mirror_shares = lax.ppermute(shares, "fs", mirror)
    far_results = apply_half(1 - own_half, rows)
    far_results, rows, mirror_target, mirror_shares = lax.optimization_barrier(
        (far_results, rows, mirror_target, mirror_shares)
    )
    far = spread(far_results)
    near_results = apply_half(own_half, rows)
    near_results, far = lax.optimization_barrier((near_results, far))
    crossing = mix(mirror_target, mirror_shares, far).astype(jnp.bfloat16)
    crossed = lax.ppermute(crossing, "fs", mirror)
    near = spread(near_results)
    mixed = mix(target, shares, near) + crossed.astype(jnp.float32)
    return (gate_serve, up_serve, down_serve, mixed.astype(jnp.bfloat16))


def solution(mesh):
    return jax.shard_map(
        on_device,
        mesh=mesh,
        in_specs=(
            P("fs", None),
            P("fs"),
            P(None, "fs", "tp"),
            P(None, "fs", "tp"),
            P(None, "fs", "tp"),
            P("fs", None),
            P("fs", None),
        ),
        out_specs=(P("fs", None, "tp"), P("fs", None, "tp"), P("fs", "tp", None), P("fs", "tp")),
        check_vma=False,
    )
```
